32 devices in a mesh: ra: 4 (over z), cb: 8 (over y, x, core).
Axes of the slice: x: 2, y: 2, z: 4, core: 2. Of those that a mesh axis runs over, the one named last changes fastest.
Arguments:
- tokens: bfloat16 [2, 128, 3072], P(None, None, 'ra'), may hold values from -70 to 70
- norm_gain: float32 [2, 3072], P(None, 'ra'), may hold values from 0.1 to 1.9
- gate_weight: float32 [2, 3072, 8448], P(None, 'ra', 'cb'), may hold values from -0.109375 to 0.109375
- gate_scale: float32 [2, 8448], P(None, 'cb'), may hold values from 0.5 to 2
- up_weight: float32 [2, 3072, 8448], P(None, 'ra', 'cb'), may hold values from -0.109375 to 0.109375
- up_scale: float32 [2, 8448], P(None, 'cb'), may hold values from 0.5 to 2
- conv_weight: float32 [2, 3, 8448], P(None, None, 'cb'), may hold values from -3.5 to 3.5
- conv_bias: float32 [2, 8448], P(None, 'cb'), may hold values from -3 to 3
- down_weight: float32 [2, 8448, 3072], P(None, 'cb', 'ra'), may hold values from -0.0625 to 0.0625
- down_scale: float32 [2, 3072], P(None, 'ra'), may hold values from 0.5 to 2
Outputs:
- layer_output: bfloat16 [2, 128, 3072], P(None, None, 'ra')
The draws below stay inside these ranges and needn't reach their ends.
All inputs are finite; a program needn't handle non-finite values.
Results may differ from the reference program's by a relative error of at most 0.014.
Values may be sent and summed in bfloat16 or wider, within the bound.
No kernel may reach another device: no remote copies, remote signals or barrier semaphores. Data moves between devices by JAX's collectives and lax.ppermute only.
A program may use at most 64 MiB of HBM per device.

```python
import math
import jax
import jax.numpy as jnp
from jax import lax

WIDTH = 3072
UNITS = 8448
KERNEL = 3
SEQUENCES = 2
LENGTH = 128


def draw_tokens(key, part):
    first, second, third = jax.random.split(key, 3)
    column_scale = jnp.exp(jnp.linspace(0.0, math.log(6.0), WIDTH)).astype(jnp.float32)
    rough = jnp.exp(jax.random.uniform(second, (WIDTH,), jnp.float32, -0.5, 0.5))
    row_scale = jnp.exp(jax.random.uniform(third, (SEQUENCES, LENGTH, 1), jnp.float32, 0.0, math.log(10.0)))
    base = jnp.clip(jax.random.normal(first, (SEQUENCES, LENGTH, WIDTH), jnp.float32), -4.0, 4.0)
    values = base * column_scale * rough * row_scale / 6.0
    return values.astype(jnp.bfloat16)


def shard_levels(key, shape, pieces, smallest, high):
    level, own = 1.0, jax.random.fold_in(key, 6)
    for position, shards_of in pieces:
        heights = jnp.exp(jax.random.uniform(jax.random.fold_in(own, position), (shards_of,), jnp.float32, smallest / len(pieces), high / len(pieces)))
        level = level * jnp.repeat(heights, shape[position] // shards_of).reshape([-1 if axis == position else 1 for axis in range(len(shape))])
    return level


def normal_values(rng, extent, deviation, most, pieces=(), held_as=jnp.bfloat16):
    gain = shard_levels(rng, extent, pieces, -0.22, 0.18) if pieces else 1.0
    drawn = jax.random.normal(rng, extent, jnp.float32) * deviation * gain
    return jnp.minimum(jnp.maximum(drawn, -most), most).astype(held_as)


def setup_inputs(seed: int = 0) -> dict:
    keys = jax.random.split(jax.random.key(seed), 11)
    tokens = draw_tokens(jax.random.fold_in(keys[10], 71), 0)
    norm_gain = jnp.clip(1.0 + 0.18 * jax.random.normal(keys[1], (2, WIDTH), jnp.float32), 0.1, 1.9)
    gate_weight = normal_values(keys[2], (2, WIDTH, UNITS), WIDTH ** -0.5, 0.109375, ((1, 4), (2, 8)), jnp.float32)
    gate_scale = jnp.clip(jnp.exp(math.log(2.0) - 1.3862944 * jax.random.uniform(keys[3], (2, UNITS), jnp.float32) ** shard_levels(keys[3], (2, UNITS), ((1, 8),), -0.2, 0.2)), 0.5, 2.0)
    up_weight = normal_values(keys[4], (2, WIDTH, UNITS), WIDTH ** -0.5, 0.109375, ((1, 4), (2, 8)), jnp.float32)
    up_scale = jnp.clip(jnp.exp(math.log(2.0) - 1.3862944 * jax.random.uniform(keys[5], (2, UNITS), jnp.float32) ** shard_levels(keys[5], (2, UNITS), ((1, 8),), -0.2, 0.2)), 0.5, 2.0)
    conv_weight = normal_values(keys[6], (2, KERNEL, UNITS), KERNEL ** -0.5, 3.5, ((2, 8),), jnp.float32)
    conv_bias = normal_values(keys[7], (2, UNITS), 0.5, 3.0, ((1, 8),), jnp.float32)
    down_weight = normal_values(keys[8], (2, UNITS, WIDTH), UNITS ** -0.5, 0.0625, ((1, 8), (2, 4)), jnp.float32)
    down_scale = jnp.clip(jnp.exp(math.log(2.0) - 1.3862944 * jax.random.uniform(keys[9], (2, WIDTH), jnp.float32) ** shard_levels(keys[9], (2, WIDTH), ((1, 4),), -0.2, 0.2)), 0.5, 2.0)
    return {"tokens": tokens, "norm_gain": norm_gain, "gate_weight": gate_weight, "gate_scale": gate_scale, "up_weight": up_weight, "up_scale": up_scale, "conv_weight": conv_weight, "conv_bias": conv_bias, "down_weight": down_weight, "down_scale": down_scale}


eps = 1e-06
residual_keep = 0.5

def causal_mix(gate_seq, conv_taps, conv_shift):
    count = conv_taps.shape[0]
    padded = jnp.pad(gate_seq, ((0, 0), (count - 1, 0), (0, 0)))
    running = jnp.zeros_like(gate_seq) + conv_shift[None, None, :]
    for offset in range(count):
        running = running + conv_taps[offset][None, None, :] * padded[:, offset:offset + LENGTH, :]
    return running

def sublayer(current, norm_g, gate_w, gate_s, up_w, up_s, conv_taps, conv_shift, down_w, down_s):
    values = current.astype(jnp.float32).reshape(SEQUENCES * LENGTH, WIDTH)
    inverse_rms = lax.rsqrt(lax.optimization_barrier(jnp.mean(values * values, axis=1, keepdims=True)) + eps)
    scaled = (values * norm_g[None, :]).astype(jnp.bfloat16)
    gate_sum = jnp.dot(scaled, gate_w.astype(jnp.bfloat16), preferred_element_type=jnp.float32)
    up_sum = jnp.dot(scaled, up_w.astype(jnp.bfloat16), preferred_element_type=jnp.float32)
    gate_sum = gate_sum * inverse_rms * gate_s[None, :]
    up_sum = up_sum * inverse_rms * up_s[None, :]
    conv_out = causal_mix(gate_sum.reshape(SEQUENCES, LENGTH, UNITS), conv_taps, conv_shift)
    hidden_act = (jax.nn.silu(conv_out) * up_sum.reshape(SEQUENCES, LENGTH, UNITS)).astype(jnp.bfloat16)
    hidden_act = hidden_act.reshape(SEQUENCES * LENGTH, UNITS)
    branch = jnp.dot(hidden_act, down_w.astype(jnp.bfloat16), preferred_element_type=jnp.float32) * down_s[None, :]
    return (residual_keep * values + branch).astype(jnp.bfloat16).reshape(SEQUENCES, LENGTH, WIDTH)

def reference(tokens, norm_gain, gate_weight, gate_scale, up_weight, up_scale, conv_weight, conv_bias, down_weight, down_scale):
    current = tokens
    for layer_index in range(2):
        current = sublayer(current, norm_gain[layer_index], gate_weight[layer_index], gate_scale[layer_index], up_weight[layer_index], up_scale[layer_index], conv_weight[layer_index], conv_bias[layer_index], down_weight[layer_index], down_scale[layer_index])
    return current
```

```python
import functools

import jax
import jax.numpy as jnp
from jax import lax
from jax.experimental import pallas as pl
from jax.experimental.pallas import tpu as pltpu
from jax.sharding import PartitionSpec as P

EPS = 1e-06
KEEP = 0.5
EXTRA = 8
F32 = jnp.float32
BF16 = jnp.bfloat16
VMEM = pltpu.VMEM
SMEM = pltpu.SMEM


def factors(count):
    found, prime = [], 2
    while count > 1:
        while count % prime == 0:
            found.append(prime)
            count //= prime
        prime += 1
    return found


def levels(count):
    stride, out = 1, []
    for size in factors(count):
        out.append((size, stride))
        stride *= size
    return out


def shift_pairs(count, size, stride, step):
    pairs = []
    for index in range(count):
        digit = index // stride % size
        pairs.append((index, index + ((digit + step) % size - digit) * stride))
    return pairs


def offsets(plan):
    grid = [()]
    for size, _ in plan:
        grid = [done + (step,) for done in grid for step in range(size)]
    return grid


def member(index, plan, steps):
    out = index
    for (size, stride), step in zip(plan, steps):
        digit = lax.rem(lax.div(index, stride), size)
        out = out + (lax.rem(digit + step, size) - digit) * stride
    return out


def rows_at(start, size, unit):
    begin = start * unit
    if unit % 8 == 0:
        begin = pl.multiple_of(begin, 8)
    return pl.ds(begin, size)


def project_kernel(plan, units, ids, own, other, gain, gate_w, up_w, *rest):
    first = plan[0][0]
    outs, (gate_acc, up_acc, sq_acc, scaled) = rest[:first], rest[first:]
    step = pl.program_id(0)
    half = own.shape[-2]
    side = ids[1]
    squares = []
    for place, source in ((side, own), (1 - side, other)):
        values = source[...].reshape(half, -1).astype(F32)
        scaled[pl.ds(pl.multiple_of(place * half, 8), half), :] = values * gain[...].reshape(1, -1)
        squares.append(values * values)
    ones = jnp.ones((8, squares[0].shape[1]), BF16)
    sq_own, sq_other = [], []
    sums = []
    for sq in squares:
        high = sq.astype(BF16)
        low = (sq - high.astype(F32)).astype(BF16)
        dims = (((1,), (1,)), ((), ()))
        sums.append(
            lax.dot_general(ones, high, dims, preferred_element_type=F32)
            + lax.dot_general(ones, low, dims, preferred_element_type=F32)
        )
    in_order = jnp.where(
        side == 0,
        jnp.concatenate(sums, axis=1),
        jnp.concatenate(sums[::-1], axis=1),
    )
    x = scaled[...].astype(BF16)
    dims = (((0,), (1,)), ((), ()))
    gate = lax.dot_general(gate_w[0].astype(BF16), x, dims, preferred_element_type=F32)
    up = lax.dot_general(up_w[0].astype(BF16), x, dims, preferred_element_type=F32)

    @pl.when(step == 0)
    def _():
        gate_acc[...] = gate
        up_acc[...] = up
        sq_acc[...] = in_order

    @pl.when(step > 0)
    def _():
        gate_acc[...] += gate
        up_acc[...] += up
        sq_acc[...] += in_order

    @pl.when(step == pl.num_programs(0) - 1)
    def _():
        total = sq_acc[...]
        high = total.astype(BF16).astype(F32)
        mid = (total - high).astype(BF16).astype(F32)
        low = total - high - mid
        row = lax.broadcasted_iota(jnp.int32, total.shape, 0)
        packed = jnp.where(row == 0, high, jnp.where(row == 1, mid, jnp.where(row == 2, low, 0.0))).astype(BF16)
        for steps in offsets(plan):
            inner = 0
            for (size, _), at in zip(plan[1:], steps[1:]):
                inner = inner * size + at
            rows = rows_at(member(ids[0], plan, steps), units, units)
            target = outs[steps[0]]
            target[inner, 0:units, :] = gate_acc[rows, :].astype(BF16)
            target[inner, units : 2 * units, :] = up_acc[rows, :].astype(BF16)
            target[inner, 2 * units : 2 * units + EXTRA, :] = packed


def project(plan, units, half, ids, halves, gain, gate_w, up_w, layer):
    count = 1
    for size, _ in plan:
        count *= size
    width, local_units = gate_w.shape[1:]
    block = 256 if width % 256 == 0 else width
    (own, own_at), (other, other_at) = halves
    rows = 2 * half
    full = lambda at: pl.BlockSpec(
        (1,) * (own.ndim - 2) + (half, block),
        lambda k, at=at: at + (k,),
    )
    first = plan[0][0]
    shape = (count // first, 2 * units + EXTRA, rows)
    return pl.pallas_call(
        functools.partial(project_kernel, plan, units),
        grid=(width // block,),
        out_shape=[jax.ShapeDtypeStruct(shape, BF16)] * first,
        in_specs=[
            pl.BlockSpec(memory_space=SMEM),
            full(own_at),
            full(other_at),
            pl.BlockSpec((1, 1, block), lambda k: (layer, 0, k)),
            pl.BlockSpec((1, block, local_units), lambda k: (layer, k, 0)),
            pl.BlockSpec((1, block, local_units), lambda k: (layer, k, 0)),
        ],
        out_specs=[pl.BlockSpec(shape, lambda k: (0, 0, 0))] * first,
        scratch_shapes=[
            VMEM((local_units, rows), F32),
            VMEM((local_units, rows), F32),
            VMEM((8, rows), F32),
            VMEM((rows, block), F32),
        ],
        cost_estimate=pl.CostEstimate(
            flops=4 * rows * width * local_units, bytes_accessed=8 * width * local_units, transcendentals=0
        ),
        name="project",
    )(ids, own, other, gain, gate_w, up_w)


def activate_kernel(units, length, width, taps, ids, params, *rest):
    parts, out = rest[:-1], rest[-1]
    total = sum(part[0].astype(F32) for part in parts[1:]) + parts[0][0].astype(F32)
    square = jnp.sum(total[2 * units :, :], axis=0, keepdims=True)
    inverse = lax.rsqrt(square / width + EPS)
    table = params[0, rows_at(ids[0], units, units), :]
    gate = total[0:units] * inverse * table[:, 0:1]
    up = total[units : 2 * units] * inverse * table[:, 1:2]
    lane = lax.rem(lax.broadcasted_iota(jnp.int32, (1, gate.shape[1]), 1), length)
    conv = table[:, 2:3] + table[:, 3 + taps - 1 : 3 + taps] * gate
    for back in range(1, taps):
        moved = jnp.where(lane >= back, pltpu.roll(gate, back, 1), 0.0)
        conv = conv + table[:, 3 + taps - 1 - back : 3 + taps - back] * moved
    out[...] = (conv / (1.0 + jnp.exp(-conv)) * up).astype(BF16)


def activate(units, length, width, taps, ids, params, parts, layer):
    rows = parts[0].shape[-1]
    block = (1,) + parts[0].shape[1:]
    return pl.pallas_call(
        functools.partial(activate_kernel, units, length, width, taps),
        grid=(1,),
        out_shape=jax.ShapeDtypeStruct((units, rows), BF16),
        in_specs=[
            pl.BlockSpec(memory_space=SMEM),
            pl.BlockSpec((1,) + params.shape[1:], lambda k: (layer, 0, 0)),
        ]
        + [pl.BlockSpec(block, lambda k: (0, 0, 0))] * len(parts),
        out_specs=pl.BlockSpec((units, rows), lambda k: (0, 0)),
        cost_estimate=pl.CostEstimate(
            flops=40 * units * rows, bytes_accessed=10 * units * rows, transcendentals=units * rows
        ),
        name="activate",
    )(ids, params, *parts)


def down_kernel(plan, units, ids, down_w, *rest):
    chunks, (keep, send, hidden, result) = rest[:-4], rest[-4:]
    for steps, chunk in zip(offsets(plan), chunks):
        hidden[rows_at(member(ids[0], plan, steps), units, units), :] = chunk[...].astype(F32)
    result[...] = lax.dot_general(
        hidden[...].astype(BF16),
        down_w[0].astype(BF16),
        (((0,), (0,)), ((), ())),
        preferred_element_type=F32,
    )
    half = keep.shape[0]
    keep[...] = result[pl.ds(pl.multiple_of(ids[1] * half, 8), half), :].astype(BF16)
    send[...] = result[pl.ds(pl.multiple_of((1 - ids[1]) * half, 8), half), :].astype(BF16)


def down(plan, units, ids, down_w, chunks, layer):
    local_units, width = down_w.shape[1:]
    rows = chunks[0].shape[-1]
    half = jax.ShapeDtypeStruct((rows // 2, width), BF16)
    return pl.pallas_call(
        functools.partial(down_kernel, plan, units),
        grid=(1,),
        out_shape=[half, half],
        in_specs=[
            pl.BlockSpec(memory_space=SMEM),
            pl.BlockSpec((1, local_units, width), lambda k: (layer, 0, 0)),
        ]
        + [pl.BlockSpec((units, rows), lambda k: (0, 0))] * len(chunks),
        out_specs=[pl.BlockSpec((rows // 2, width), lambda k: (0, 0))] * 2,
        scratch_shapes=[VMEM((local_units, rows), F32), VMEM((rows, width), F32)],
        cost_estimate=pl.CostEstimate(
            flops=2 * rows * width * local_units, bytes_accessed=4 * width * local_units, transcendentals=0
        ),
        name="down",
    )(ids, down_w, *chunks)


def make_shards(mesh, groups):
    ra, cb = mesh.shape["ra"], mesh.shape["cb"]
    ra_plan = levels(ra)
    cb_plan = levels(cb)
    inner = cb_plan[0]

    def send_ra(x, level, step):
        return lax.ppermute(x, "ra", shift_pairs(ra, *level, step))

    def send_cb(x, level, step=1):
        return lax.ppermute(x, "cb", shift_pairs(cb, *level, step))

    def scatter_sum(parts):
        kept, arrived = parts[0], [send_ra(parts[k], ra_plan[0], k) for k in range(1, ra_plan[0][0])]
        mine = [kept] + arrived
        for depth in range(1, len(ra_plan)):
            size, _ = ra_plan[depth]
            per = mine[0].shape[0] // size
            later = []
            for step in range(1, size):
                block = sum(m[step * per : (step + 1) * per].astype(F32) for m in mine).astype(BF16)
                later.append(send_ra(block, ra_plan[depth], step))
            if per > 1:
                head = sum(m[:per].astype(F32) for m in mine)
                mine = [head.astype(BF16)] + later
            else:
                mine = mine + later
        return mine

    def gather(hidden):
        have = [hidden]
        for level in ra_plan[::-1]:
            have = have + [send_ra(x, level, step) for step in range(1, level[0]) for x in have]
        return have

    def sum_cb(keep, send):
        total = keep.astype(F32) + send_cb(send, inner).astype(F32)
        for level in cb_plan[1:]:
            mine = total.astype(BF16)
            total = mine.astype(F32)
            for step in range(1, level[0]):
                total = total + send_cb(mine, level, step).astype(F32)
        return total

    def shards(tokens, norm_gain, gate_w, gate_s, up_w, up_s, conv_w, conv_b, down_w, down_s):
        layers = gate_w.shape[0]
        sequences, length, local_width = tokens.shape
        width = local_width * ra
        units = gate_w.shape[2] // ra
        taps = conv_w.shape[1]
        me, side = lax.axis_index("ra"), lax.rem(lax.axis_index("cb"), 2)
        ids = jnp.stack([me, side]).astype(jnp.int32)
        first_ids = jnp.stack([me, 0 * side]).astype(jnp.int32)
        params = jnp.concatenate([gate_s[:, None], up_s[:, None], conv_b[:, None], conv_w], axis=1)
        params = jnp.transpose(params, (0, 2, 1))
        gain = norm_gain[:, None, :]
        half = length // 2
        own_tokens = lax.dynamic_slice_in_dim(tokens, side * half, half, 1)
        state = [None] * sequences
        own = [own_tokens[s] for s in range(sequences)]
        for layer in range(layers):
            for s in range(sequences):
                if layer == 0:
                    halves, used = ((tokens, (s, 0)), (tokens, (s, 1))), first_ids
                else:
                    halves, used = ((own[s], (0,)), (state[s], (0,))), ids
                parts = project(ra_plan, units, half, used, halves, gain, gate_w, up_w, layer)
                mine = scatter_sum(parts)
                hidden = activate(units, length, width, taps, ids, params, mine, layer)
                chunks = gather(hidden)
                order = gather_order(ra_plan)
                keep, send = down(ra_plan, units, ids, down_w, [chunks[order.index(o)] for o in offsets(ra_plan)], layer)
                total = sum_cb(keep, send) * down_s[layer][None, :]
                own[s] = (KEEP * own[s].astype(F32) + total).astype(BF16)
                state[s] = send_cb(own[s], inner)
        outs = []
        for s in range(sequences):
            low = jnp.where(side == 0, own[s], state[s])
            high = jnp.where(side == 0, state[s], own[s])
            outs.append(jnp.concatenate([low, high], axis=0))
        return jnp.stack(outs)

    return shards


def gather_order(plan):
    have = [(0,) * len(plan)]
    for depth in range(len(plan) - 1, -1, -1):
        size = plan[depth][0]
        have = have + [
            item[:depth] + ((item[depth] - step) % size,) + item[depth + 1 :]
            for step in range(1, size)
            for item in have
        ]
    return have


def solution(mesh):
    in_specs = (
        P(None, None, "ra"),
        P(None, "ra"),
        P(None, "ra", "cb"),
        P(None, "cb"),
        P(None, "ra", "cb"),
        P(None, "cb"),
        P(None, None, "cb"),
        P(None, "cb"),
        P(None, "cb", "ra"),
        P(None, "ra"),
    )
    return jax.shard_map(
        make_shards(mesh, 2), mesh=mesh, in_specs=in_specs, out_specs=P(None, None, "ra"), check_vma=False
    )
```

```python
import functools

import jax
import jax.numpy as jnp
from jax import lax
from jax.experimental import pallas as pl
from jax.experimental.pallas import tpu as pltpu
from jax.sharding import PartitionSpec as P

EPS = 1e-06
KEEP = 0.5
EXTRA = 8
F32 = jnp.float32
BF16 = jnp.bfloat16
VMEM = pltpu.VMEM
SMEM = pltpu.SMEM


def factors(count):
    found, prime = [], 2
    while count > 1:
        while count % prime == 0:
            found.append(prime)
            count //= prime
        prime += 1
    return found


def levels(count):
    stride, out = 1, []
    for size in factors(count):
        out.append((size, stride))
        stride *= size
    return out


def shift_pairs(count, size, stride, step):
    pairs = []
    for index in range(count):
        digit = index // stride % size
        pairs.append((index, index + ((digit + step) % size - digit) * stride))
    return pairs


def offsets(plan):
    grid = [()]
    for size, _ in plan:
        grid = [done + (step,) for done in grid for step in range(size)]
    return grid


def member(index, plan, steps):
    out = index
    for (size, stride), step in zip(plan, steps):
        digit = lax.rem(lax.div(index, stride), size)
        out = out + (lax.rem(digit + step, size) - digit) * stride
    return out


def rows_at(start, size, unit):
    begin = start * unit
    if unit % 8 == 0:
        begin = pl.multiple_of(begin, 8)
    return pl.ds(begin, size)


def project_kernel(plan, layer, units, half, groups, ids, own, other, gain, gate_w, up_w, *rest):
    first = plan[0][0]
    outs, (scaled, packed) = rest[:-2], rest[-2:]
    step = pl.program_id(0)
    side = ids[1]
    wide = ((1,), (1,)), ((), ())

    @pl.when(step == 0)
    def _():
        for group, (own_at, other_at) in enumerate(groups):
            sums = []
            for place, source, at in ((side, own, own_at), (1 - side, other, other_at)):
                values = source[at].astype(F32)
                rows = pl.ds(pl.multiple_of(place * half, 8), half)
                scaled[group, rows, :] = values * gain[layer : layer + 1, :]
                squares = values * values
                high = squares.astype(BF16)
                low = (squares - high.astype(F32)).astype(BF16)
                ones = jnp.ones((8, values.shape[1]), BF16)
                sums.append(
                    lax.dot_general(ones, high, wide, preferred_element_type=F32)
                    + lax.dot_general(ones, low, wide, preferred_element_type=F32)
                )
            total = jnp.where(
                side == 0,
                jnp.concatenate(sums, axis=1),
                jnp.concatenate(sums[::-1], axis=1),
            )
            high = total.astype(BF16).astype(F32)
            mid = (total - high).astype(BF16).astype(F32)
            low = total - high - mid
            row = lax.broadcasted_iota(jnp.int32, total.shape, 0)
            packed[group] = jnp.where(row == 0, high, jnp.where(row == 1, mid, jnp.where(row == 2, low, 0.0)))

    rows = 2 * half
    x = scaled[...].reshape(len(groups) * rows, -1).astype(BF16)
    gate = lax.dot_general(gate_w[0, 0].astype(BF16), x, wide, preferred_element_type=F32).astype(BF16)
    up = lax.dot_general(up_w[0, 0].astype(BF16), x, wide, preferred_element_type=F32).astype(BF16)
    for place, steps in enumerate(offsets(plan)):
        inner = 0
        for (size, _), at in zip(plan[1:], steps[1:]):
            inner = inner * size + at

        @pl.when(step == place)
        def _():
            for group in range(len(groups)):
                target = outs[group * first + steps[0]]
                lanes = slice(group * rows, (group + 1) * rows)
                target[inner, 0:units, :] = gate[:, lanes]
                target[inner, units : 2 * units, :] = up[:, lanes]
                target[inner, 2 * units : 2 * units + EXTRA, :] = packed[group].astype(BF16)


def chunk_at(plan, place, ids):
    steps = []
    for size, _ in plan[::-1]:
        steps.append(lax.rem(place, size))
        place = lax.div(place, size)
    return member(ids[0], plan, steps[::-1])


def project(plan, half, ids, own, other, groups, gain, gate_w, up_w, layer):
    _, count, units, width = gate_w.shape
    rows = 2 * half
    first = plan[0][0]
    shape = (count // first, 2 * units + EXTRA, rows)
    weight = pl.BlockSpec((1, 1, units, width), lambda j, ids: (layer, chunk_at(plan, j, ids), 0, 0))
    whole = pl.BlockSpec(memory_space=VMEM)
    number = len(groups) * first
    return pl.pallas_call(
        functools.partial(project_kernel, plan, layer, units, half, groups),
        grid_spec=pltpu.PrefetchScalarGridSpec(
            num_scalar_prefetch=1,
            grid=(count,),
            in_specs=[whole, whole, whole, weight, weight],
            out_specs=[pl.BlockSpec(shape, lambda j, ids: (0, 0, 0))] * number,
            scratch_shapes=[VMEM((len(groups), rows, width), F32), VMEM((len(groups), EXTRA, rows), F32)],
        ),
        out_shape=[jax.ShapeDtypeStruct(shape, BF16)] * number,
        compiler_params=pltpu.CompilerParams(vmem_limit_bytes=16 << 20),
        cost_estimate=pl.CostEstimate(
            flops=4 * rows * width * count * units, bytes_accessed=8 * width * count * units, transcendentals=0
        ),
        name="project",
    )(ids, own, other, gain, gate_w, up_w)


def activate_kernel(layer, units, length, width, taps, params, *rest):
    parts, out = rest[:-1], rest[-1]
    total = sum(part[0].astype(F32) for part in parts)
    square = jnp.sum(total[2 * units :, :], axis=0, keepdims=True)
    inverse = lax.rsqrt(square / width + EPS)
    table = params[layer]
    gate = total[0:units] * inverse * table[:, 0:1]
    up = total[units : 2 * units] * inverse * table[:, 1:2]
    lane = lax.rem(lax.broadcasted_iota(jnp.int32, (1, gate.shape[1]), 1), length)
    conv = table[:, 2:3] + table[:, 3 + taps - 1 : 3 + taps] * gate
    for back in range(1, taps):
        moved = jnp.where(lane >= back, pltpu.roll(gate, back, 1), 0.0)
        conv = conv + table[:, 3 + taps - 1 - back : 3 + taps - back] * moved
    out[...] = (conv / (1.0 + jnp.exp(-conv)) * up).astype(BF16)


def activate(units, length, width, taps, params, parts, layer):
    rows = parts[0].shape[-1]
    whole = pl.BlockSpec(memory_space=VMEM)
    return pl.pallas_call(
        functools.partial(activate_kernel, layer, units, length, width, taps),
        out_shape=jax.ShapeDtypeStruct((units, rows), BF16),
        in_specs=[whole] * (1 + len(parts)),
        out_specs=whole,
        compiler_params=pltpu.CompilerParams(vmem_limit_bytes=8 << 20),
        cost_estimate=pl.CostEstimate(
            flops=40 * units * rows, bytes_accessed=10 * units * rows, transcendentals=units * rows
        ),
        name="activate",
    )(params, *parts)


def down_kernel(plan, units, ids, down_w, *rest):
    chunks, (keep, send, hidden, result) = rest[:-4], rest[-4:]
    for steps, chunk in zip(offsets(plan), chunks):
        hidden[rows_at(member(ids[0], plan, steps), units, units), :] = chunk[...].astype(F32)
    result[...] = lax.dot_general(
        hidden[...].astype(BF16),
        down_w[0].astype(BF16),
        (((0,), (0,)), ((), ())),
        preferred_element_type=F32,
    )
    half = keep.shape[0]
    keep[...] = result[pl.ds(pl.multiple_of(ids[1] * half, 8), half), :].astype(BF16)
    send[...] = result[pl.ds(pl.multiple_of((1 - ids[1]) * half, 8), half), :].astype(BF16)


def down(plan, units, ids, down_w, chunks, layer):
    local_units, width = down_w.shape[1:]
    rows = chunks[0].shape[-1]
    half = jax.ShapeDtypeStruct((rows // 2, width), BF16)
    whole = pl.BlockSpec(memory_space=VMEM)
    return pl.pallas_call(
        functools.partial(down_kernel, plan, units),
        grid=(1,),
        out_shape=[half, half],
        in_specs=[
            pl.BlockSpec(memory_space=SMEM),
            pl.BlockSpec((1, local_units, width), lambda k: (layer, 0, 0)),
        ]
        + [whole] * len(chunks),
        out_specs=[whole] * 2,
        scratch_shapes=[VMEM((local_units, rows), F32), VMEM((rows, width), F32)],
        compiler_params=pltpu.CompilerParams(vmem_limit_bytes=16 << 20),
        cost_estimate=pl.CostEstimate(
            flops=2 * rows * width * local_units, bytes_accessed=4 * width * local_units, transcendentals=0
        ),
        name="down",
    )(ids, down_w, *chunks)


def make_shards(mesh, groups):
    ra, cb = mesh.shape["ra"], mesh.shape["cb"]
    ra_plan = levels(ra)
    cb_plan = levels(cb)
    inner = cb_plan[0]

    def send_ra(x, level, step):
        return lax.ppermute(x, "ra", shift_pairs(ra, *level, step))

    def send_cb(x, level, step=1):
        return lax.ppermute(x, "cb", shift_pairs(cb, *level, step))

    def scatter_sum(parts):
        kept, arrived = parts[0], [send_ra(parts[k], ra_plan[0], k) for k in range(1, ra_plan[0][0])]
        mine = [kept] + arrived
        for depth in range(1, len(ra_plan)):
            size, _ = ra_plan[depth]
            per = mine[0].shape[0] // size
            later = []
            for step in range(1, size):
                block = sum(m[step * per : (step + 1) * per].astype(F32) for m in mine).astype(BF16)
                later.append(send_ra(block, ra_plan[depth], step))
            if per > 1:
                head = sum(m[:per].astype(F32) for m in mine)
                mine = [head.astype(BF16)] + later
            else:
                mine = mine + later
        return mine

    def gather(hidden):
        have = [hidden]
        for level in ra_plan[::-1]:
            have = have + [send_ra(x, level, step) for step in range(1, level[0]) for x in have]
        return have

    def sum_cb(keep, send):
        total = keep.astype(F32) + send_cb(send, inner).astype(F32)
        for level in cb_plan[1:]:
            mine = total.astype(BF16)
            total = mine.astype(F32)
            for step in range(1, level[0]):
                total = total + send_cb(mine, level, step).astype(F32)
        return total

    def shards(tokens, norm_gain, gate_w, gate_s, up_w, up_s, conv_w, conv_b, down_w, down_s):
        layers = gate_w.shape[0]
        sequences, length, local_width = tokens.shape
        width = local_width * ra
        units = gate_w.shape[2] // ra
        taps = conv_w.shape[1]
        me, side = lax.axis_index("ra"), lax.rem(lax.axis_index("cb"), 2)
        ids = jnp.stack([me, side]).astype(jnp.int32)
        first_ids = jnp.stack([me, 0 * side]).astype(jnp.int32)
        params = jnp.concatenate([gate_s[:, None], up_s[:, None], conv_b[:, None], conv_w], axis=1)
        params = jnp.transpose(params, (0, 2, 1))
        params = lax.dynamic_slice_in_dim(params, me * units, units, 1)
        half = length // 2
        by_chunk = lambda w: jnp.swapaxes(w, 1, 2).reshape(layers, ra, units, local_width)
        gate_t, up_t = by_chunk(gate_w), by_chunk(up_w)
        order = gather_order(ra_plan)
        own_tokens = lax.dynamic_slice_in_dim(tokens, side * half, half, 1)
        own = [own_tokens[s] for s in range(sequences)]
        other = [None] * sequences
        first = ra_plan[0][0]
        groups = [((s, slice(0, half)), (s, slice(half, 2 * half))) for s in range(sequences)]
        started = project(ra_plan, half, first_ids, tokens, tokens, groups, norm_gain, gate_t, up_t, 0)
        for layer in range(layers):
            for s in range(sequences):
                if layer == 0:
                    parts = started[s * first : (s + 1) * first]
                else:
                    groups = [(slice(None), slice(None))]
                    parts = project(ra_plan, half, ids, own[s], other[s], groups, norm_gain, gate_t, up_t, layer)
                mine = scatter_sum(parts)
                hidden = activate(units, length, width, taps, params, mine, layer)
                chunks = gather(hidden)
                chunks = [chunks[order.index(steps)] for steps in offsets(ra_plan)]
                keep, send = down(ra_plan, units, ids, down_w, chunks, layer)
                total = sum_cb(keep, send) * down_s[layer][None, :]
                own[s] = (KEEP * own[s].astype(F32) + total).astype(BF16)
                other[s] = send_cb(own[s], inner)
        outs = []
        for s in range(sequences):
            low = jnp.where(side == 0, own[s], other[s])
            high = jnp.where(side == 0, other[s], own[s])
            outs.append(jnp.concatenate([low, high], axis=0))
        return jnp.stack(outs)

    return shards


def gather_order(plan):
    have = [(0,) * len(plan)]
    for depth in range(len(plan) - 1, -1, -1):
        size = plan[depth][0]
        have = have + [
            item[:depth] + ((item[depth] - step) % size,) + item[depth + 1 :]
            for step in range(1, size)
            for item in have
        ]
    return have


def solution(mesh):
    in_specs = (
        P(None, None, "ra"),
        P(None, "ra"),
        P(None, "ra", "cb"),
        P(None, "cb"),
        P(None, "ra", "cb"),
        P(None, "cb"),
        P(None, None, "cb"),
        P(None, "cb"),
        P(None, "cb", "ra"),
        P(None, "ra"),
    )
    return jax.shard_map(
        make_shards(mesh, 2), mesh=mesh, in_specs=in_specs, out_specs=P(None, None, "ra"), check_vma=False
    )
```
